128 devices in a mesh: grp: 4 (over y, x), ep: 32 (over z, core).
Axes of the slice: x: 2, y: 2, z: 16, core: 2. Of those that a mesh axis runs over, the one named last changes fastest.
The devices are a block of a 8x8x16 slice.
Arguments:
- tokens: bfloat16 [65536, 2048], P(('grp', 'ep')), parts along dimension 0, may hold values from -6 to 6
- norm_gain: float32 [2048], replicated, may hold values from 0.1 to 1.9
- route_ids: int32 [65536, 2], P(('grp', 'ep')), parts along dimension 0, may hold values from 0 to 31, all different within a row; in each aligned block of 512 rows (0 to 511, 512 to 1023, ...) at most 48 rows name the same one
- route_gates: float32 [65536, 2], P(('grp', 'ep')), parts along dimension 0, may hold values from 0.05 to 1
- w_gate: bfloat16 [32, 2048, 1024], P('ep'), may hold values from -0.125 to 0.125
- w_up: bfloat16 [32, 2048, 1024], P('ep'), may hold values from -0.125 to 0.125
- w_down: bfloat16 [32, 1024, 2048], P('ep'), may hold values from -0.1875 to 0.1875
Outputs:
- mixed: bfloat16 [65536, 2048], P(('grp', 'ep')), parts along dimension 0
The draws below stay inside these ranges and needn't reach their ends.
There are 4 independent parts, one for each index of `grp`. The reference program is written for one: setup_inputs(seed, part) draws one part's arguments, and reference() takes and returns one part's arrays. A program takes and returns all parts, laid end to end along the dimension named above; an argument that names none is the same for every part. Nothing has to cross between parts.
Inputs may be any that keep to these rules, and one draw needn't show every extreme that they name: `route_ids`: each row names 2 different experts. Among the rows of one device no expert is named more than 48 times, and in some devices' rows one expert is named exactly 48 times.
All inputs are finite; a program needn't handle non-finite values.
Results may differ from the reference program's by a relative error of at most 0.0071.
Values may be sent and summed in bfloat16 or wider, within the bound.
No kernel may reach another device: no remote copies, remote signals or barrier semaphores. Data moves between devices by JAX's collectives and lax.ppermute only.
A program may use at most 128 MiB of HBM per device.

```python
import math
import jax
import jax.numpy as jnp
import numpy as np
from jax import lax

D = 2048
FF = 1024
TOPK = 2
TOK_DEV = 512
EXPERTS = 32
CAP = 48
TOKENS = 16384
N_EP = 32


def steps_of(rng, dims, split, low, top_value):
    level = 1.0
    for axis_at, parts in split:
        draws = jax.random.uniform(jax.random.fold_in(jax.random.fold_in(rng, 6), axis_at), (parts,), jnp.float32, low / len(split), top_value / len(split))
        level = level * jnp.repeat(jnp.exp(draws), dims[axis_at] // parts).reshape((-1,) + (1,) * (len(dims) - 1 - axis_at))
    return level


def shared_out(key, own, number, rows, number_of, top, most, slope):
    sequence = jax.random.permutation(key, number_of)
    packed, common = shares(number_of, rows * top, most, slope, True), shares(number_of, rows * top, most, slope, False)
    places = jnp.arange(number_of)

    def named(lengths, offset_by):
        used = int((lengths > 0).sum())
        fixed = max(1, used // 4)
        shifted = fixed + (places - fixed + offset_by * (used - fixed)) % max(1, number_of - fixed)
        return jnp.zeros((number_of,), jnp.int32).at[sequence[jnp.where(places < fixed, places, shifted)]].set(jnp.asarray(lengths, jnp.int32))

    lengths = jnp.where(number % 4 == 0, named(packed, number // 4), named(common, number - number // 4 - 1))
    mixed = jax.random.permutation(jax.random.fold_in(own, 3), number_of)
    giver, sink = mixed[0:number_of // 2 * 2:2], mixed[1:number_of // 2 * 2:2]
    slack = jnp.minimum(lengths[giver] - 1, most - lengths[sink]) // 2
    slack = jnp.where((giver == sequence[0]) | (sink == sequence[0]) | (lengths[sink] == 0), 0, jnp.maximum(slack, 0))
    shifted = jax.random.randint(jax.random.fold_in(own, 4), (number_of // 2,), 0, 1 << 20) % (slack + 1)
    lengths = lengths.at[giver].add(-shifted).at[sink].add(shifted)
    labels = jnp.searchsorted(jnp.cumsum(lengths), jnp.arange(rows * top), side="right").astype(jnp.int32)
    listing = labels.reshape(top, rows).T
    listing = listing[jax.random.permutation(jax.random.fold_in(own, 1), rows)]
    offset_by = jax.random.randint(jax.random.fold_in(own, 2), (rows, 1), 0, top)
    return jnp.take_along_axis(listing, (jnp.arange(top)[None, :] + offset_by) % top, axis=1)


def shares(number_of, total, most, slope, full):
    weights = [(1 << 20) // math.isqrt(rank ** slope) + 1 for rank in range(1, number_of + 1)]
    largest = most if full else min(most, max(-(-total // number_of), total * weights[0] // sum(weights)))
    least = 1 if total - largest >= number_of - 1 else 0
    counts, rest = [largest] + [least] * (number_of - 1), total - largest - least * (number_of - 1)
    while rest > 0:
        movable = [i for i in range(1, number_of) if counts[i] < largest] or [i for i in range(1, number_of) if counts[i] < most]
        mass, remaining = sum([weights[i] for i in movable]), rest
        for i in movable:
            extra = min(most - counts[i], max(1, remaining * weights[i] // mass), rest)
            counts[i] = counts[i] + extra
            rest = rest - extra
    return np.array(counts)


def scatter_about(own_key, shape, spread, limit, shards=(), held_as=jnp.bfloat16):
    array = jax.random.normal(own_key, shape, jnp.float32) * spread
    if len(shards) > 0:
        array = steps_of(own_key, shape, shards, -0.22, 0.18) * array
    return jnp.clip(array, min=-limit, max=limit).astype(held_as)


def setup_inputs(seed: int = 0, part: int = 0) -> dict:
    streams_of = jax.random.split(jax.random.key(seed), 8)
    part_splits = jax.random.split(jax.random.fold_in(streams_of[7], part), 8)
    tokens = scatter_about(part_splits[0], (TOKENS, D), 1.0, 6.0, ((0, 32),))
    norm_gain = jnp.clip(1.0 + 0.18 * jax.random.normal(streams_of[1], (D,), jnp.float32), 0.1, 1.9)
    route_ids_keys = jax.random.split(jax.random.fold_in(part_splits[2], 1), TOKENS // TOK_DEV)
    route_ids_turns = jax.random.permutation(jax.random.fold_in(part_splits[2], 3), TOKENS // TOK_DEV)
    route_ids = jax.vmap(lambda own, number: shared_out(jax.random.fold_in(part_splits[2], 2), own, number, TOK_DEV, EXPERTS, TOPK, CAP, 2))(route_ids_keys, route_ids_turns).reshape((TOKENS, TOPK))
    route_gates = jnp.clip(0.05 + 0.95 * jax.random.uniform(part_splits[3], (TOKENS, TOPK), jnp.float32) ** steps_of(part_splits[3], (TOKENS, TOPK), ((0, 32),), -0.2, 0.2), 0.05, 1.0)
    w_gate = scatter_about(streams_of[4], (EXPERTS, D, FF), D ** -0.5, 0.125, ((0, 32),))
    w_up = scatter_about(streams_of[5], (EXPERTS, D, FF), D ** -0.5, 0.125, ((0, 32),))
    w_down = scatter_about(streams_of[6], (EXPERTS, FF, D), FF ** -0.5, 0.1875, ((0, 32),))
    return dict(tokens=tokens, norm_gain=norm_gain, route_ids=route_ids, route_gates=route_gates, w_gate=w_gate, w_up=w_up, w_down=w_down)


EPS = 1e-06

def reference(tokens, norm_gain, route_ids, route_gates, w_gate, w_up, w_down):
    floats = tokens.astype(jnp.float32)
    scale = lax.rsqrt(lax.optimization_barrier(jnp.mean(floats * floats, axis=-1, keepdims=True)) + EPS)
    normed = (floats * scale * norm_gain).astype(jnp.bfloat16)
    weights = route_gates / lax.optimization_barrier(jnp.sum(route_gates, axis=-1, keepdims=True))
    count = TOKENS * TOPK
    flat_ids = route_ids.reshape(-1)
    flat_weights = weights.reshape(-1)
    most = N_EP * CAP

    def one_expert(carry, inputs):
        expert, gate_mat, up_mat, down_mat = inputs
        picked = jnp.nonzero(flat_ids == expert, size=most, fill_value=count)[0].astype(jnp.int32)
        live = picked < count
        pairs = jnp.minimum(picked, count - 1)
        rows = pairs // TOPK
        chosen = normed[rows]
        gate_pre = jnp.dot(chosen, gate_mat, preferred_element_type=jnp.float32)
        up_pre = jnp.dot(chosen, up_mat, preferred_element_type=jnp.float32)
        hidden = (jax.nn.silu(gate_pre) * up_pre).astype(jnp.bfloat16)
        result = jnp.dot(hidden, down_mat, preferred_element_type=jnp.float32).astype(jnp.bfloat16)
        factor = jnp.where(live, flat_weights[pairs], jnp.zeros_like(flat_weights[pairs]))
        return (carry.at[rows].add(result.astype(jnp.float32) * factor[:, None]), None)
    start = jnp.zeros((TOKENS, D), jnp.float32)
    total, _ = lax.scan(one_expert, start, (jnp.arange(EXPERTS, dtype=jnp.int32), w_gate, w_up, w_down))
    return total.astype(jnp.bfloat16)
```

```python
import jax
import jax.numpy as jnp
from jax import lax
from jax.sharding import PartitionSpec as P

EPS = 1e-06
BF16, F32 = jnp.bfloat16, jnp.float32


def rms_norm(tokens, norm_gain):
    floats = tokens.astype(F32)
    scale = lax.rsqrt(jnp.mean(floats * floats, axis=-1, keepdims=True) + EPS)
    return (floats * scale * norm_gain).astype(BF16)


def dot(a, b):
    return jnp.dot(a, b, preferred_element_type=F32)


def ranks_of(route_ids, experts):
    rows = route_ids.shape[0]
    names = route_ids[:, :, None] == jnp.arange(experts, dtype=jnp.int32)
    member = jnp.any(names, axis=1)
    earlier = jnp.arange(rows)[:, None] > jnp.arange(rows)[None, :]
    return names, dot(earlier.astype(BF16), member.astype(BF16)).astype(jnp.int32)


def split_weight(weight):
    high = weight.astype(BF16)
    return high, (weight - high.astype(F32)).astype(BF16)


def expert_rows(rows, w_gate, w_up, w_down):
    gate_pre, up_pre = dot(rows, w_gate[0]), dot(rows, w_up[0])
    hidden = (jax.nn.silu(gate_pre) * up_pre).astype(BF16)
    return dot(hidden, w_down[0]).astype(BF16)


def body(tokens, norm_gain, route_ids, route_gates, w_gate, w_up, w_down):
    tok_rows, width = tokens.shape
    top_count = route_ids.shape[1]
    experts = lax.axis_size("ep") * w_gate.shape[0]
    capacity = 3 * tok_rows * top_count // (2 * experts)
    normed = rms_norm(tokens, norm_gain)
    weights = route_gates / jnp.sum(route_gates, axis=1, keepdims=True)
    names, ranks = ranks_of(route_ids, experts)
    places = route_ids * capacity + jnp.sum(names * ranks[:, None, :], axis=2)
    slots = jnp.arange(experts * capacity, dtype=jnp.int32)
    hits = [slots[:, None] == places[None, :, k] for k in range(top_count)]
    pick = sum(hit.astype(BF16) for hit in hits)
    outgoing = dot(pick, normed).astype(BF16)
    arrived = lax.all_to_all(outgoing.reshape(experts, capacity, width), "ep", split_axis=0, concat_axis=0, tiled=True)
    finished = expert_rows(arrived.reshape(experts * capacity, width), w_gate, w_up, w_down)
    returned = lax.all_to_all(finished.reshape(experts, capacity, width), "ep", split_axis=0, concat_axis=0, tiled=True)
    returned = returned.reshape(experts * capacity, width)
    high, low = split_weight(weights)
    spread = lambda part: sum(
        jnp.where(places[:, k : k + 1] == slots[None, :], part[:, k : k + 1], 0) for k in range(top_count)
    )
    return (dot(spread(high), returned) + dot(spread(low), returned)).astype(BF16)


def solution(mesh):
    rows = P(("grp", "ep"), None)
    by_expert = P("ep", None, None)
    placed = (rows, P(), rows, rows, by_expert, by_expert, by_expert)
    return jax.shard_map(body, mesh=mesh, in_specs=placed, out_specs=rows, check_vma=False)
```

```python
import jax
import jax.numpy as jnp
import numpy as np
from jax import lax
from jax.sharding import PartitionSpec as P


EPS = 1e-06
BF16, F32, I32 = jnp.bfloat16, jnp.float32, jnp.int32
CORES = 2
HOPS = (528, 480, 424, 368, 328, 264, 224, 144, 80)
NEAR = 4
PARTS = 2
HOLD = 8
BATCHES = ((1, 2, 3, 4), (5, 6, 7, 8, 9))
WAYS = (1, -1)


def rms_norm(tokens, norm_gain):
    floats = tokens.astype(F32)
    scale = lax.rsqrt(jnp.mean(floats * floats, axis=-1, keepdims=True) + EPS)
    return (floats * scale * norm_gain).astype(BF16)


def dot(a, b):
    return jnp.dot(a, b, preferred_element_type=F32)


def ranks_of(ids, experts):
    rows = ids.shape[0]
    names = ids[:, :, None] == jnp.arange(experts, dtype=I32)
    member = jnp.any(names, axis=1)
    earlier = jnp.arange(rows)[:, None] > jnp.arange(rows)[None, :]
    return names, member, dot(earlier.astype(BF16), member.astype(BF16)).astype(I32)


def pick_of(places, slots):
    at = jnp.arange(slots, dtype=I32)[:, None]
    return sum((at == places[None, :, k]).astype(BF16) for k in range(places.shape[1]))


def mix(places, weights, values):
    at = jnp.arange(values.shape[0], dtype=I32)[None, :]
    spread = sum(jnp.where(places[:, k : k + 1] == at, weights[:, k : k + 1], 0) for k in range(places.shape[1]))
    return dot(spread.astype(BF16), values)


def expert_rows(rows, w_gate, w_up, w_down):
    gate_pre, up_pre = dot(rows, w_gate[0]), dot(rows, w_up[0])
    hidden = (jax.nn.silu(gate_pre) * up_pre).astype(BF16)
    return dot(hidden, w_down[0]).astype(BF16)


def direct(normed, weights, ids, capacity, w_gate, w_up, w_down):
    width = normed.shape[1]
    experts = lax.axis_size("ep")
    names, _, ranks = ranks_of(ids, experts)
    places = ids * capacity + jnp.sum(names * ranks[:, None, :], axis=2)
    outgoing = dot(pick_of(places, experts * capacity), normed).astype(BF16)
    arrived = lax.all_to_all(outgoing.reshape(experts, capacity, width), "ep", split_axis=0, concat_axis=0, tiled=True)
    finished = expert_rows(arrived.reshape(experts * capacity, width), w_gate, w_up, w_down)
    returned = lax.all_to_all(finished.reshape(experts, capacity, width), "ep", split_axis=0, concat_axis=0, tiled=True)
    return mix(places, weights, returned.reshape(experts * capacity, width)).astype(BF16)


def body(tokens, norm_gain, route_ids, route_gates, w_gate, w_up, w_down):
    tok_rows, width = tokens.shape
    top_count = route_ids.shape[1]
    experts = lax.axis_size("ep")
    chips = experts // CORES
    capacity = 3 * tok_rows * top_count // (2 * experts)
    far = len(HOPS)
    fixed = HOPS[NEAR]
    me = lax.axis_index("ep")
    chip, core = lax.div(me, CORES), lax.rem(me, CORES)
    step = {
        way: [(z * CORES + c, (z + way) % chips * CORES + c) for z in range(chips) for c in range(CORES)]
        for way in WAYS
    }
    swap = [(i, i ^ 1) for i in range(experts)]
    columns = [slice(part * width // PARTS, (part + 1) * width // PARTS) for part in range(PARTS)]
    hop = lambda block, way: lax.ppermute(block, "ep", step[way])

    near = lax.rem(route_ids + (experts - chip * CORES), experts)
    names, member, ranks = ranks_of(near, experts)
    order = jnp.arange(experts)
    count = jnp.sum(member.astype(I32) * (order >= CORES), axis=0)
    after = jnp.sum(jnp.where(order[None, :] <= order[:, None], count[None, :], 0), axis=1)
    before = after - count
    above, below = np.full(experts, 1 << 20, np.int32), np.full(experts, -(1 << 20), np.int32)
    last = lambda chips_on: CORES * chips_on + CORES - 1
    above[last(far)], below[last(chips - 1 - far)] = 0, 0
    for k, rows in enumerate(HOPS, 1):
        above[last(k - 1)], below[last(chips - k)] = rows, -rows
    most, least = jnp.min(after + above), jnp.max(after + below)
    cut = lax.shift_right_logical(least + most, 1)
    spilt = least > most

    rank = jnp.sum(names * ranks[:, None, :], axis=2)
    seat = rank + jnp.sum(names * before, axis=2)
    local = near < CORES
    places = {
        1: jnp.where(~local & (seat < cut), cut - 1 - seat, -1),
        -1: jnp.where(~local & (seat >= cut), seat - cut, -1),
        0: jnp.where(local, jnp.where(near == core, 0, capacity) + rank, -1),
    }

    normed = rms_norm(tokens, norm_gain)
    weights = route_gates / jnp.sum(route_gates, axis=1, keepdims=True)
    first = lambda way, low, high: dot(pick_of(places[way] - low, high - low), normed).astype(BF16)
    near_block = {way: first(way, fixed, HOPS[0]) for way in WAYS}
    far_block = {}
    for way in WAYS:
        block = first(way, 0, fixed)
        for part in range(PARTS):
            far_block[way, part] = block[:, columns[part]]
    here = first(0, 0, 2 * capacity)

    sent = [jnp.maximum(jnp.minimum(after, cut) - before, 0), jnp.maximum(after - jnp.maximum(before, cut), 0)]
    row = jnp.concatenate(sent + [jnp.full((experts,), spilt, I32)]).astype(F32)
    table = lax.all_to_all(
        jnp.broadcast_to(row, (experts, row.shape[0])), "ep", split_axis=0, concat_axis=0, tiled=True
    )
    spilt = jnp.max(table[:, 2 * experts]) > 0
    hops = jnp.arange(1, far + 1, dtype=I32)
    slot = jnp.arange(capacity, dtype=F32)
    wants = {}
    for i, way in enumerate(WAYS):
        source = lax.rem(chip - way * hops + chips, chips) * CORES + core
        mine = (source[:, None] == order[None, :]).astype(F32)
        counts = jnp.dot(mine, table[:, i * experts : (i + 1) * experts], precision=lax.Precision.HIGHEST)
        aim = CORES * hops if way > 0 else CORES * (chips - hops)
        parts = []
        for to in (core, 1 - core):
            ahead = order[None, :] > aim[:, None] + to if way > 0 else order[None, :] < aim[:, None] + to
            start = jnp.sum(jnp.where(ahead, counts, 0), axis=1)
            size = jnp.sum(jnp.where(order[None, :] == aim[:, None] + to, counts, 0), axis=1)
            parts.append(jnp.where(slot[None, :] < size[:, None], start[:, None] + slot[None, :], -1))
        wants[way] = jnp.concatenate(parts, axis=1)

    def run(got):
        own = jnp.concatenate([g[:capacity] for g in got])
        other = jnp.concatenate([g[capacity:] for g in got])
        n = own.shape[0]
        done = expert_rows(jnp.concatenate([own, lax.ppermute(other, "ep", swap)]), w_gate, w_up, w_down)
        back = lax.ppermute(done[n:], "ep", swap)
        span = lambda i: slice(i * capacity, (i + 1) * capacity)
        return [jnp.concatenate([done[span(i)], back[span(i)]]) for i in range(len(got))]

    def pick(way, k, low, high):
        return (wants[way][k - 1][:, None] == jnp.arange(low, high, dtype=F32)[None, :]).astype(BF16)

    far_at, near_at = {}, {}
    for k in range(1, far + 1):
        for way in WAYS:
            if k <= NEAR:
                near_block[way] = near_at[way, k] = hop(near_block[way][: HOPS[k - 1] - fixed], way)
        for part in range(PARTS):
            for way in WAYS:
                block = hop(far_block[way, part][: min(fixed, HOPS[k - 1])], way)
                far_block[way, part] = far_at[way, k, part] = block

    def select(way, k):
        rows = min(fixed, HOPS[k - 1])
        got = []
        for part in range(PARTS):
            got.append(dot(pick(way, k, 0, rows), far_at[way, k, part]))
        got = jnp.concatenate(got, axis=1)
        if k <= NEAR:
            got = got + dot(pick(way, k, fixed, HOPS[k - 1]), near_at[way, k])
        return got.astype(BF16)

    outs = {}
    for batch in BATCHES:
        keys = [(way, k) for k in batch for way in WAYS]
        got = [select(way, k) for way, k in keys]
        if batch is BATCHES[0]:
            keys.append((0, 0))
            got.append(here)
        outs.update(zip(keys, run(got)))

    held, held_near = {}, {}
    for k in range(NEAR, 0, -1):
        for way in WAYS:
            put = dot(pick(way, k, fixed, HOPS[k - 1]).T, outs[way, k]).astype(BF16)
            if k < NEAR:
                put = put + jnp.pad(held_near[way], ((0, HOPS[k - 1] - HOPS[k]), (0, 0)))
            elif HOLD:
                put, _ = lax.optimization_barrier((put, far_at[way, HOLD, 0]))
            held_near[way] = hop(put, -way)
    for k in range(far, 0, -1):
        rows = min(fixed, HOPS[k - 1])
        for part in range(PARTS):
            for way in WAYS:
                put = dot(pick(way, k, 0, rows).T, outs[way, k][:, columns[part]]).astype(BF16)
                if k < far:
                    got = held[way, part]
                    put = put + jnp.pad(got, ((0, rows - got.shape[0]), (0, 0)))
                held[way, part] = hop(put, -way)

    early = mix(places[0], weights, outs[0, 0])
    for way in WAYS:
        early = early + mix(places[way] - fixed, weights, held_near[way])
    total = []
    for part in range(PARTS):
        last_sum = early[:, columns[part]]
        for way in WAYS:
            last_sum = last_sum + mix(places[way], weights, held[way, part])
        total.append(last_sum.astype(BF16))
    quick = jnp.concatenate(total, axis=1)
    return lax.cond(
        spilt,
        lambda: direct(normed, weights, route_ids, capacity, w_gate, w_up, w_down),
        lambda: quick,
    )


def solution(mesh):
    rows = P(("grp", "ep"), None)
    by_expert = P("ep", None, None)
    placed = (rows, P(), rows, rows, by_expert, by_expert, by_expert)

    return jax.shard_map(body, mesh=mesh, in_specs=placed, out_specs=rows, check_vma=False)
```

```python
import jax
import jax.numpy as jnp
import numpy as np
from jax import lax
from jax.sharding import PartitionSpec as P


EPS = 1e-06
BF16, F32, I32 = jnp.bfloat16, jnp.float32, jnp.int32
CORES = 2
HOPS = (528, 480, 424, 368, 328, 264, 224, 144, 80)
NEAR = 4
PARTS = 2
HOLD = 7
BATCHES = ((1, 2, 3, 4), (5, 6, 7, 8, 9))
WAYS = (1, -1)


def rms_norm(tokens, norm_gain):
    floats = tokens.astype(F32)
    scale = lax.rsqrt(jnp.mean(floats * floats, axis=-1, keepdims=True) + EPS)
    return (floats * scale * norm_gain).astype(BF16)


def dot(a, b):
    return jnp.dot(a, b, preferred_element_type=F32)


def ranks_of(ids, experts):
    rows = ids.shape[0]
    names = ids[:, :, None] == jnp.arange(experts, dtype=I32)
    member = jnp.any(names, axis=1)
    earlier = jnp.arange(rows)[:, None] > jnp.arange(rows)[None, :]
    return names, member, dot(earlier.astype(BF16), member.astype(BF16)).astype(I32)


def pick_of(places, slots):
    at = jnp.arange(slots, dtype=I32)[:, None]
    return sum((at == places[None, :, k]).astype(BF16) for k in range(places.shape[1]))


def mix(places, weights, values):
    at = jnp.arange(values.shape[0], dtype=I32)[None, :]
    spread = sum(jnp.where(places[:, k : k + 1] == at, weights[:, k : k + 1], 0) for k in range(places.shape[1]))
    return dot(spread.astype(BF16), values)


def expert_rows(rows, w_gate, w_up, w_down):
    gate_pre = dot(rows, w_gate[0])
    up_pre = dot(rows, w_up[0])
    hidden = (jax.nn.silu(gate_pre) * up_pre).astype(BF16)
    return dot(hidden, w_down[0]).astype(BF16)


def direct(normed, weights, ids, capacity, w_gate, w_up, w_down):
    width = normed.shape[1]
    experts = lax.axis_size("ep")
    names, _, ranks = ranks_of(ids, experts)
    places = ids * capacity + jnp.sum(names * ranks[:, None, :], axis=2)
    outgoing = dot(pick_of(places, experts * capacity), normed).astype(BF16)
    arrived = lax.all_to_all(outgoing.reshape(experts, capacity, width), "ep", split_axis=0, concat_axis=0, tiled=True)
    finished = expert_rows(arrived.reshape(experts * capacity, width), w_gate, w_up, w_down)
    returned = lax.all_to_all(finished.reshape(experts, capacity, width), "ep", split_axis=0, concat_axis=0, tiled=True)
    return mix(places, weights, returned.reshape(experts * capacity, width)).astype(BF16)


def body(tokens, norm_gain, route_ids, route_gates, w_gate, w_up, w_down):
    tok_rows, width = tokens.shape
    top_count = route_ids.shape[1]
    experts = lax.axis_size("ep")
    chips = experts // CORES
    capacity = 3 * tok_rows * top_count // (2 * experts)
    far = len(HOPS)
    fixed = HOPS[NEAR]
    me = lax.axis_index("ep")
    chip, core = lax.div(me, CORES), lax.rem(me, CORES)
    step = {
        way: [(z * CORES + c, (z + way) % chips * CORES + c) for z in range(chips) for c in range(CORES)]
        for way in WAYS
    }
    swap = [(i, i ^ 1) for i in range(experts)]
    columns = [slice(part * width // PARTS, (part + 1) * width // PARTS) for part in range(PARTS)]
    hop = lambda block, way: lax.ppermute(block, "ep", step[way])

    near = lax.rem(route_ids + (experts - chip * CORES), experts)
    names, member, ranks = ranks_of(near, experts)
    order = jnp.arange(experts)
    count = jnp.sum(member.astype(I32) * (order >= CORES), axis=0)
    after = jnp.sum(jnp.where(order[None, :] <= order[:, None], count[None, :], 0), axis=1)
    before = after - count
    above, below = np.full(experts, 1 << 20, np.int32), np.full(experts, -(1 << 20), np.int32)
    last = lambda chips_on: CORES * chips_on + CORES - 1
    above[last(far)], below[last(chips - 1 - far)] = 0, 0
    for k, rows in enumerate(HOPS, 1):
        above[last(k - 1)], below[last(chips - k)] = rows, -rows
    most, least = jnp.min(after + above), jnp.max(after + below)
    cut = lax.shift_right_logical(least + most, 1)
    spilt = least > most

    rank = jnp.sum(names * ranks[:, None, :], axis=2)
    seat = rank + jnp.sum(names * before, axis=2)
    local = near < CORES
    places = {
        1: jnp.where(~local & (seat < cut), cut - 1 - seat, -1),
        -1: jnp.where(~local & (seat >= cut), seat - cut, -1),
        0: jnp.where(local, jnp.where(near == core, 0, capacity) + rank, -1),
    }

    normed = rms_norm(tokens, norm_gain)
    weights = route_gates / jnp.sum(route_gates, axis=1, keepdims=True)
    first = lambda way, low, high: dot(pick_of(places[way] - low, high - low), normed).astype(BF16)
    near_block = {way: first(way, fixed, HOPS[0]) for way in WAYS}
    far_block = {}
    for way in WAYS:
        block = first(way, 0, fixed)
        for part in range(PARTS):
            far_block[way, part] = block[:, columns[part]]
    here = first(0, 0, 2 * capacity)

    far_at, near_at = {}, {}
    for k in range(1, far + 1):
        for way in WAYS:
            if k <= NEAR:
                near_block[way] = near_at[way, k] = hop(near_block[way][: HOPS[k - 1] - fixed], way)
        for part in range(PARTS):
            for way in WAYS:
                block = hop(far_block[way, part][: min(fixed, HOPS[k - 1])], way)
                far_block[way, part] = far_at[way, k, part] = block

    sent = [jnp.maximum(jnp.minimum(after, cut) - before, 0), jnp.maximum(after - jnp.maximum(before, cut), 0)]
    row = jnp.concatenate(sent + [jnp.full((experts,), spilt, I32)]).astype(F32)
    row, _ = lax.optimization_barrier((jnp.broadcast_to(row, (experts, row.shape[0])), near_at[1, 1]))
    table = lax.all_to_all(row, "ep", split_axis=0, concat_axis=0, tiled=True)
    spilt = jnp.max(table[:, 2 * experts]) > 0
    hops = jnp.arange(1, far + 1, dtype=I32)
    slot = jnp.arange(capacity, dtype=F32)
    wants = {}
    for i, way in enumerate(WAYS):
        source = lax.rem(chip - way * hops + chips, chips) * CORES + core
        mine = (source[:, None] == order[None, :]).astype(F32)
        counts = jnp.dot(mine, table[:, i * experts : (i + 1) * experts], precision=lax.Precision.HIGHEST)
        aim = CORES * hops if way > 0 else CORES * (chips - hops)
        parts = []
        for to in (core, 1 - core):
            ahead = order[None, :] > aim[:, None] + to if way > 0 else order[None, :] < aim[:, None] + to
            start = jnp.sum(jnp.where(ahead, counts, 0), axis=1)
            size = jnp.sum(jnp.where(order[None, :] == aim[:, None] + to, counts, 0), axis=1)
            parts.append(jnp.where(slot[None, :] < size[:, None], start[:, None] + slot[None, :], -1))
        wants[way] = jnp.concatenate(parts, axis=1)

    def run(got):
        own = jnp.concatenate([g[:capacity] for g in got])
        other = jnp.concatenate([g[capacity:] for g in got])
        n = own.shape[0]
        other = lax.ppermute(other, "ep", swap)
        done = expert_rows(jnp.concatenate([own, other]), w_gate, w_up, w_down)
        back = lax.ppermute(done[n:], "ep", swap)
        span = lambda i: slice(i * capacity, (i + 1) * capacity)
        return [jnp.concatenate([done[span(i)], back[span(i)]]) for i in range(len(got))]

    def pick(way, k, low, high):
        return (wants[way][k - 1][:, None] == jnp.arange(low, high, dtype=F32)[None, :]).astype(BF16)

    def select(way, k):
        rows = min(fixed, HOPS[k - 1])
        got = []
        for part in range(PARTS):
            got.append(dot(pick(way, k, 0, rows), far_at[way, k, part]))
        got = jnp.concatenate(got, axis=1)
        if k <= NEAR:
            got = got + dot(pick(way, k, fixed, HOPS[k - 1]), near_at[way, k])
        return got.astype(BF16)

    outs = {}
    for batch in BATCHES:
        keys = [(way, k) for k in batch for way in WAYS]
        got = [select(way, k) for way, k in keys]
        if batch is BATCHES[0]:
            keys.append((0, 0))
            got.append(here)
        outs.update(zip(keys, run(got)))

    held, held_near = {}, {}
    for k in range(NEAR, 0, -1):
        for way in WAYS:
            put = dot(pick(way, k, fixed, HOPS[k - 1]).T, outs[way, k]).astype(BF16)
            if k < NEAR:
                put = put + jnp.pad(held_near[way], ((0, HOPS[k - 1] - HOPS[k]), (0, 0)))
            elif HOLD:
                put, _ = lax.optimization_barrier((put, far_at[way, HOLD, 0]))
            held_near[way] = hop(put, -way)
    for k in range(far, 0, -1):
        rows = min(fixed, HOPS[k - 1])
        for part in range(PARTS):
            for way in WAYS:
                put = dot(pick(way, k, 0, rows).T, outs[way, k][:, columns[part]]).astype(BF16)
                if k < far:
                    got = held[way, part]
                    put = put + jnp.pad(got, ((0, rows - got.shape[0]), (0, 0)))
                held[way, part] = hop(put, -way)

    early = mix(places[0], weights, outs[0, 0])
    for way in WAYS:
        early = early + mix(places[way] - fixed, weights, held_near[way])
    total = []
    for part in range(PARTS):
        last_sum = early[:, columns[part]]
        for way in WAYS:
            last_sum = last_sum + mix(places[way], weights, held[way, part])
        total.append(last_sum.astype(BF16))
    quick = jnp.concatenate(total, axis=1)
    return lax.cond(
        spilt,
        lambda: direct(normed, weights, route_ids, capacity, w_gate, w_up, w_down),
        lambda: quick,
    )


def solution(mesh):
    rows = P(("grp", "ep"), None)
    by_expert = P("ep", None, None)
    placed = (rows, P(), rows, rows, by_expert, by_expert, by_expert)

    return jax.shard_map(body, mesh=mesh, in_specs=placed, out_specs=rows, check_vma=False)
```

```python
import jax
import jax.numpy as jnp
import numpy as np
from jax import lax
from jax.sharding import PartitionSpec as P


EPS = 1e-06
BF16, F32, I32 = jnp.bfloat16, jnp.float32, jnp.int32
CORES = 2
HOPS = (528, 480, 424, 368, 328, 264, 224, 144, 80)
NEAR = 4
PARTS = 2
BATCHES = ((1, 2, 3, 4), (5, 6, 7, 8, 9))
WAYS = (1, -1)


def rms_norm(tokens, norm_gain):
    floats = tokens.astype(F32)
    scale = lax.rsqrt(jnp.mean(floats * floats, axis=-1, keepdims=True) + EPS)
    return (floats * scale * norm_gain).astype(BF16)


def dot(a, b):
    return jnp.dot(a, b, preferred_element_type=F32)


def ranks_of(ids, experts):
    rows = ids.shape[0]
    names = ids[:, :, None] == jnp.arange(experts, dtype=I32)
    member = jnp.any(names, axis=1)
    earlier = jnp.arange(rows)[:, None] > jnp.arange(rows)[None, :]
    return names, member, dot(earlier.astype(BF16), member.astype(BF16)).astype(I32)


def pick_of(places, slots):
    at = jnp.arange(slots, dtype=I32)[:, None]
    return sum((at == places[None, :, k]).astype(BF16) for k in range(places.shape[1]))


def mix(places, weights, values):
    at = jnp.arange(values.shape[0], dtype=I32)[None, :]
    spread = sum(jnp.where(places[:, k : k + 1] == at, weights[:, k : k + 1], 0) for k in range(places.shape[1]))
    return dot(spread.astype(BF16), values)


def expert_rows(rows, w_gate, w_up, w_down):
    gate_pre = dot(rows, w_gate[0])
    up_pre = dot(rows, w_up[0])
    hidden = (jax.nn.silu(gate_pre) * up_pre).astype(BF16)
    return dot(hidden, w_down[0]).astype(BF16)


def direct(normed, weights, ids, capacity, w_gate, w_up, w_down):
    width = normed.shape[1]
    experts = lax.axis_size("ep")
    names, _, ranks = ranks_of(ids, experts)
    places = ids * capacity + jnp.sum(names * ranks[:, None, :], axis=2)
    outgoing = dot(pick_of(places, experts * capacity), normed).astype(BF16)
    arrived = lax.all_to_all(outgoing.reshape(experts, capacity, width), "ep", split_axis=0, concat_axis=0, tiled=True)
    finished = expert_rows(arrived.reshape(experts * capacity, width), w_gate, w_up, w_down)
    returned = lax.all_to_all(finished.reshape(experts, capacity, width), "ep", split_axis=0, concat_axis=0, tiled=True)
    return mix(places, weights, returned.reshape(experts * capacity, width)).astype(BF16)


def body(tokens, norm_gain, route_ids, route_gates, w_gate, w_up, w_down):
    tok_rows, width = tokens.shape
    top_count = route_ids.shape[1]
    experts = lax.axis_size("ep")
    chips = experts // CORES
    capacity = 3 * tok_rows * top_count // (2 * experts)
    far = len(HOPS)
    fixed = HOPS[NEAR]
    me = lax.axis_index("ep")
    chip, core = lax.div(me, CORES), lax.rem(me, CORES)
    step = {
        way: [(z * CORES + c, (z + way) % chips * CORES + c) for z in range(chips) for c in range(CORES)]
        for way in WAYS
    }
    swap = [(i, i ^ 1) for i in range(experts)]
    columns = [slice(part * width // PARTS, (part + 1) * width // PARTS) for part in range(PARTS)]
    hop = lambda block, way: lax.ppermute(block, "ep", step[way])

    near = lax.rem(route_ids + (experts - chip * CORES), experts)
    names, member, ranks = ranks_of(near, experts)
    order = jnp.arange(experts)
    count = jnp.sum(member.astype(I32) * (order >= CORES), axis=0)
    after = jnp.sum(jnp.where(order[None, :] <= order[:, None], count[None, :], 0), axis=1)
    before = after - count
    above, below = np.full(experts, 1 << 20, np.int32), np.full(experts, -(1 << 20), np.int32)
    last = lambda chips_on: CORES * chips_on + CORES - 1
    above[last(far)], below[last(chips - 1 - far)] = 0, 0
    for k, rows in enumerate(HOPS, 1):
        above[last(k - 1)], below[last(chips - k)] = rows, -rows
    most, least = jnp.min(after + above), jnp.max(after + below)
    cut = lax.shift_right_logical(least + most, 1)
    spilt = least > most

    rank = jnp.sum(names * ranks[:, None, :], axis=2)
    seat = rank + jnp.sum(names * before, axis=2)
    local = near < CORES
    places = {
        1: jnp.where(~local & (seat < cut), cut - 1 - seat, -1),
        -1: jnp.where(~local & (seat >= cut), seat - cut, -1),
        0: jnp.where(local, jnp.where(near == core, 0, capacity) + rank, -1),
    }

    normed = rms_norm(tokens, norm_gain)
    weights = route_gates / jnp.sum(route_gates, axis=1, keepdims=True)
    first = lambda way, low, high: dot(pick_of(places[way] - low, high - low), normed).astype(BF16)
    near_block = {way: first(way, fixed, HOPS[0]) for way in WAYS}
    far_block = {}
    for way in WAYS:
        block = first(way, 0, fixed)
        for part in range(PARTS):
            far_block[way, part] = block[:, columns[part]]
    here = first(0, 0, 2 * capacity)

    far_at, near_at = {}, {}
    for k in range(1, far + 1):
        for way in WAYS:
            if k <= NEAR:
                near_block[way] = near_at[way, k] = hop(near_block[way][: HOPS[k - 1] - fixed], way)
        for part in range(PARTS):
            for way in WAYS:
                block = hop(far_block[way, part][: min(fixed, HOPS[k - 1])], way)
                far_block[way, part] = far_at[way, k, part] = block

    sent = [jnp.maximum(jnp.minimum(after, cut) - before, 0), jnp.maximum(after - jnp.maximum(before, cut), 0)]
    row = jnp.concatenate(sent + [jnp.full((experts,), spilt, I32)]).astype(F32)
    row = jnp.broadcast_to(row, (experts, row.shape[0]))
    table = lax.all_to_all(row, "ep", split_axis=0, concat_axis=0, tiled=True)
    table, _ = lax.optimization_barrier((table, far_at[1, 2, 0]))
    spilt = jnp.max(table[:, 2 * experts]) > 0
    hops = jnp.arange(1, far + 1, dtype=I32)
    slot = jnp.arange(capacity, dtype=F32)
    wants = {}
    for i, way in enumerate(WAYS):
        source = lax.rem(chip - way * hops + chips, chips) * CORES + core
        mine = (source[:, None] == order[None, :]).astype(F32)
        counts = jnp.dot(mine, table[:, i * experts : (i + 1) * experts], precision=lax.Precision.HIGHEST)
        aim = CORES * hops if way > 0 else CORES * (chips - hops)
        parts = []
        for to in (core, 1 - core):
            ahead = order[None, :] > aim[:, None] + to if way > 0 else order[None, :] < aim[:, None] + to
            start = jnp.sum(jnp.where(ahead, counts, 0), axis=1)
            size = jnp.sum(jnp.where(order[None, :] == aim[:, None] + to, counts, 0), axis=1)
            parts.append(jnp.where(slot[None, :] < size[:, None], start[:, None] + slot[None, :], -1))
        wants[way] = jnp.concatenate(parts, axis=1)

    def run(got):
        own = jnp.concatenate([g[:capacity] for g in got])
        other = jnp.concatenate([g[capacity:] for g in got])
        n = own.shape[0]
        other = lax.ppermute(other, "ep", swap)
        done = expert_rows(jnp.concatenate([own, other]), w_gate, w_up, w_down)
        back = lax.ppermute(done[n:], "ep", swap)
        span = lambda i: slice(i * capacity, (i + 1) * capacity)
        return [jnp.concatenate([done[span(i)], back[span(i)]]) for i in range(len(got))]

    def pick(way, k, low, high):
        return (wants[way][k - 1][:, None] == jnp.arange(low, high, dtype=F32)[None, :]).astype(BF16)

    def select(way, k):
        rows = min(fixed, HOPS[k - 1])
        got = []
        for part in range(PARTS):
            got.append(dot(pick(way, k, 0, rows), far_at[way, k, part]))
        got = jnp.concatenate(got, axis=1)
        if k <= NEAR:
            got = got + dot(pick(way, k, fixed, HOPS[k - 1]), near_at[way, k])
        return got.astype(BF16)

    outs = {}
    for batch in BATCHES:
        keys = [(way, k) for k in batch for way in WAYS]
        got = [select(way, k) for way, k in keys]
        if batch is BATCHES[0]:
            keys.append((0, 0))
            got.append(here)
        outs.update(zip(keys, run(got)))

    held, held_near = {}, {}
    for k in range(NEAR, 0, -1):
        for way in WAYS:
            put = dot(pick(way, k, fixed, HOPS[k - 1]).T, outs[way, k]).astype(BF16)
            if k < NEAR:
                put = put + jnp.pad(held_near[way], ((0, HOPS[k - 1] - HOPS[k]), (0, 0)))
            held_near[way] = hop(put, -way)
    for k in range(far, 0, -1):
        rows = min(fixed, HOPS[k - 1])
        for part in range(PARTS):
            for way in WAYS:
                put = dot(pick(way, k, 0, rows).T, outs[way, k][:, columns[part]]).astype(BF16)
                if k < far:
                    got = held[way, part]
                    put = put + jnp.pad(got, ((0, rows - got.shape[0]), (0, 0)))
                held[way, part] = hop(put, -way)
        if k == NEAR:
            held_near, _ = lax.optimization_barrier((held_near, held[1, 0]))

    early = mix(places[0], weights, outs[0, 0])
    for way in WAYS:
        early = early + mix(places[way] - fixed, weights, held_near[way])
    total = []
    for part in range(PARTS):
        last_sum = early[:, columns[part]]
        for way in WAYS:
            last_sum = last_sum + mix(places[way], weights, held[way, part])
        total.append(last_sum.astype(BF16))
    quick = jnp.concatenate(total, axis=1)
    return lax.cond(
        spilt,
        lambda: direct(normed, weights, route_ids, capacity, w_gate, w_up, w_down),
        lambda: quick,
    )


def solution(mesh):
    rows = P(("grp", "ep"), None)
    by_expert = P("ep", None, None)
    placed = (rows, P(), rows, rows, by_expert, by_expert, by_expert)

    return jax.shard_map(body, mesh=mesh, in_specs=placed, out_specs=rows, check_vma=False)
```

```python
import jax
import jax.numpy as jnp
import numpy as np
from jax import lax
from jax.sharding import PartitionSpec as P


EPS = 1e-06
BF16, F32, I32 = jnp.bfloat16, jnp.float32, jnp.int32
CORES = 2
HOPS = (528, 480, 424, 368, 328, 264, 224, 144, 80)
NEAR = 4
PARTS = 2
BATCHES = ((1, 2, 3, 4), (5, 6, 7, 8, 9))
WAYS = (1, -1)


def rms_norm(tokens, norm_gain):
    floats = tokens.astype(F32)
    scale = lax.rsqrt(jnp.mean(floats * floats, axis=-1, keepdims=True) + EPS)
    return (floats * scale * norm_gain).astype(BF16)


def dot(a, b):
    return jnp.dot(a, b, preferred_element_type=F32)


def ranks_of(ids, experts):
    rows = ids.shape[0]
    names = ids[:, :, None] == jnp.arange(experts, dtype=I32)
    member = jnp.any(names, axis=1)
    earlier = jnp.arange(rows)[:, None] > jnp.arange(rows)[None, :]
    return names, member, dot(earlier.astype(BF16), member.astype(BF16)).astype(I32)


def pick_of(places, slots):
    at = jnp.arange(slots, dtype=I32)[:, None]
    return sum((at == places[None, :, k]).astype(BF16) for k in range(places.shape[1]))


def mix(places, weights, values):
    at = jnp.arange(values.shape[0], dtype=I32)[None, :]
    spread = sum(jnp.where(places[:, k : k + 1] == at, weights[:, k : k + 1], 0) for k in range(places.shape[1]))
    return dot(spread.astype(BF16), values)


def expert_rows(rows, w_gate, w_up, w_down):
    gate_pre = dot(rows, w_gate[0])
    up_pre = dot(rows, w_up[0])
    hidden = (jax.nn.silu(gate_pre) * up_pre).astype(BF16)
    return dot(hidden, w_down[0]).astype(BF16)


def direct(normed, weights, ids, capacity, w_gate, w_up, w_down):
    width = normed.shape[1]
    experts = lax.axis_size("ep")
    names, _, ranks = ranks_of(ids, experts)
    places = ids * capacity + jnp.sum(names * ranks[:, None, :], axis=2)
    outgoing = dot(pick_of(places, experts * capacity), normed).astype(BF16)
    arrived = lax.all_to_all(outgoing.reshape(experts, capacity, width), "ep", split_axis=0, concat_axis=0, tiled=True)
    finished = expert_rows(arrived.reshape(experts * capacity, width), w_gate, w_up, w_down)
    returned = lax.all_to_all(finished.reshape(experts, capacity, width), "ep", split_axis=0, concat_axis=0, tiled=True)
    return mix(places, weights, returned.reshape(experts * capacity, width)).astype(BF16)


def body(tokens, norm_gain, route_ids, route_gates, w_gate, w_up, w_down):
    tok_rows, width = tokens.shape
    top_count = route_ids.shape[1]
    experts = lax.axis_size("ep")
    chips = experts // CORES
    capacity = 3 * tok_rows * top_count // (2 * experts)
    far = len(HOPS)
    fixed = HOPS[NEAR]
    me = lax.axis_index("ep")
    chip, core = lax.div(me, CORES), lax.rem(me, CORES)
    step = {
        way: [(z * CORES + c, (z + way) % chips * CORES + c) for z in range(chips) for c in range(CORES)]
        for way in WAYS
    }
    swap = [(i, i ^ 1) for i in range(experts)]
    columns = [slice(part * width // PARTS, (part + 1) * width // PARTS) for part in range(PARTS)]
    hop = lambda block, way: lax.ppermute(block, "ep", step[way])

    near = lax.rem(route_ids + (experts - chip * CORES), experts)
    names, member, ranks = ranks_of(near, experts)
    order = jnp.arange(experts)
    count = jnp.sum(member.astype(I32) * (order >= CORES), axis=0)
    after = jnp.sum(jnp.where(order[None, :] <= order[:, None], count[None, :], 0), axis=1)
    before = after - count
    above, below = np.full(experts, 1 << 20, np.int32), np.full(experts, -(1 << 20), np.int32)
    last = lambda chips_on: CORES * chips_on + CORES - 1
    above[last(far)], below[last(chips - 1 - far)] = 0, 0
    for k, rows in enumerate(HOPS, 1):
        above[last(k - 1)], below[last(chips - k)] = rows, -rows
    most, least = jnp.min(after + above), jnp.max(after + below)
    cut = lax.shift_right_logical(least + most, 1)
    spilt = least > most

    rank = jnp.sum(names * ranks[:, None, :], axis=2)
    seat = rank + jnp.sum(names * before, axis=2)
    local = near < CORES
    places = {
        1: jnp.where(~local & (seat < cut), cut - 1 - seat, -1),
        -1: jnp.where(~local & (seat >= cut), seat - cut, -1),
        0: jnp.where(local, jnp.where(near == core, 0, capacity) + rank, -1),
    }

    normed = rms_norm(tokens, norm_gain)
    weights = route_gates / jnp.sum(route_gates, axis=1, keepdims=True)

    def first(way, low, high, span=slice(None)):
        return dot(pick_of(places[way] - low, high - low), normed[:, span]).astype(BF16)

    near_block = {way: first(way, fixed, HOPS[0]) for way in WAYS}
    far_block = {}
    for way in WAYS:
        for part in range(PARTS):
            far_block[way, part] = first(way, 0, fixed, columns[part])
    here = first(0, 0, 2 * capacity)

    far_at, near_at = {}, {}
    for k in range(1, far + 1):
        for way in WAYS:
            if k <= NEAR:
                near_block[way] = near_at[way, k] = hop(near_block[way][: HOPS[k - 1] - fixed], way)
        for part in range(PARTS):
            for way in WAYS:
                block = hop(far_block[way, part][: min(fixed, HOPS[k - 1])], way)
                far_block[way, part] = far_at[way, k, part] = block

    sent = [jnp.maximum(jnp.minimum(after, cut) - before, 0), jnp.maximum(after - jnp.maximum(before, cut), 0)]
    row = jnp.concatenate(sent + [jnp.full((experts,), spilt, I32)]).astype(F32)
    row = jnp.broadcast_to(row, (experts, row.shape[0]))
    table = lax.all_to_all(row, "ep", split_axis=0, concat_axis=0, tiled=True)
    table, _ = lax.optimization_barrier((table, far_at[1, 2, 0]))
    spilt = jnp.max(table[:, 2 * experts]) > 0
    hops = jnp.arange(1, far + 1, dtype=I32)
    slot = jnp.arange(capacity, dtype=F32)
    wants = {}
    for i, way in enumerate(WAYS):
        source = lax.rem(chip - way * hops + chips, chips) * CORES + core
        mine = (source[:, None] == order[None, :]).astype(F32)
        counts = jnp.dot(mine, table[:, i * experts : (i + 1) * experts], precision=lax.Precision.HIGHEST)
        aim = CORES * hops if way > 0 else CORES * (chips - hops)
        parts = []
        for to in (core, 1 - core):
            ahead = order[None, :] > aim[:, None] + to if way > 0 else order[None, :] < aim[:, None] + to
            start = jnp.sum(jnp.where(ahead, counts, 0), axis=1)
            size = jnp.sum(jnp.where(order[None, :] == aim[:, None] + to, counts, 0), axis=1)
            parts.append(jnp.where(slot[None, :] < size[:, None], start[:, None] + slot[None, :], -1))
        wants[way] = jnp.concatenate(parts, axis=1)

    def run(got):
        own = jnp.concatenate([g[:capacity] for g in got])
        other = jnp.concatenate([g[capacity:] for g in got])
        n = own.shape[0]
        other = lax.ppermute(other, "ep", swap)
        done = expert_rows(jnp.concatenate([own, other]), w_gate, w_up, w_down)
        back = lax.ppermute(done[n:], "ep", swap)
        span = lambda i: slice(i * capacity, (i + 1) * capacity)
        return [jnp.concatenate([done[span(i)], back[span(i)]]) for i in range(len(got))]

    def pick(way, k, low, high):
        return (wants[way][k - 1][:, None] == jnp.arange(low, high, dtype=F32)[None, :]).astype(BF16)

    def select(way, k):
        rows = min(fixed, HOPS[k - 1])
        got = []
        for part in range(PARTS):
            got.append(dot(pick(way, k, 0, rows), far_at[way, k, part]))
        got = jnp.concatenate(got, axis=1)
        if k <= NEAR:
            got = got + dot(pick(way, k, fixed, HOPS[k - 1]), near_at[way, k])
        return got.astype(BF16)

    outs = {}
    for batch in BATCHES:
        keys = [(way, k) for k in batch for way in WAYS]
        got = [select(way, k) for way, k in keys]
        if batch is BATCHES[0]:
            keys.append((0, 0))
            got.append(here)
        outs.update(zip(keys, run(got)))

    held, held_near = {}, {}
    for k in range(NEAR, 0, -1):
        for way in WAYS:
            put = dot(pick(way, k, fixed, HOPS[k - 1]).T, outs[way, k]).astype(BF16)
            if k < NEAR:
                put = put + jnp.pad(held_near[way], ((0, HOPS[k - 1] - HOPS[k]), (0, 0)))
            held_near[way] = hop(put, -way)
    for k in range(far, 0, -1):
        rows = min(fixed, HOPS[k - 1])
        for part in range(PARTS):
            for way in WAYS:
                put = dot(pick(way, k, 0, rows).T, outs[way, k][:, columns[part]]).astype(BF16)
                if k < far:
                    got = held[way, part]
                    put = put + jnp.pad(got, ((0, rows - got.shape[0]), (0, 0)))
                held[way, part] = hop(put, -way)
        if k == NEAR:
            held_near, _ = lax.optimization_barrier((held_near, held[1, 0]))

    early = mix(places[0], weights, outs[0, 0])
    for way in WAYS:
        early = early + mix(places[way] - fixed, weights, held_near[way])
    total = []
    for part in range(PARTS):
        last_sum = early[:, columns[part]]
        for way in WAYS:
            last_sum = last_sum + mix(places[way], weights, held[way, part])
        total.append(last_sum.astype(BF16))
    quick = jnp.concatenate(total, axis=1)
    return lax.cond(
        spilt,
        lambda: direct(normed, weights, route_ids, capacity, w_gate, w_up, w_down),
        lambda: quick,
    )


def solution(mesh):
    rows = P(("grp", "ep"), None)
    by_expert = P("ep", None, None)
    placed = (rows, P(), rows, rows, by_expert, by_expert, by_expert)

    return jax.shard_map(body, mesh=mesh, in_specs=placed, out_specs=rows, check_vma=False)
```
